1024 devices in a mesh: fs: 128 (over z, y), tp: 8 (over x, core).
Axes of the slice: x: 4, y: 4, z: 32, core: 2. Of those that a mesh axis runs over, the one named last changes fastest.
Arguments:
- tokens: bfloat16 [49152, 2048], P('fs'), may hold values from -6 to 6
- first_norm_scale: float32 [2048], replicated, may hold values from 0.1 to 1.9
- recurrent_branch_matrix: bfloat16 [2048, 1024], P('fs', 'tp'), may hold values from -0.125 to 0.125
- gelu_gate_matrix: bfloat16 [2048, 1024], P('fs', 'tp'), may hold values from -0.125 to 0.125
- filter_taps_weight: bfloat16 [4, 1024], P(None, 'tp'), may hold values from -3 to 3
- recurrence_gate_blocks: bfloat16 [16, 64, 64], P('tp'), may hold values from -0.75 to 0.75
- input_gate_blocks: bfloat16 [16, 64, 64], P('tp'), may hold values from -0.75 to 0.75
- base_decay_logits: float32 [1024], P('tp'), may hold values from 4 to 11
- extra_log_decay: float32 [49152, 1024], P('fs', 'tp'), may hold values from -0.7 to 0
- mixer_output_matrix: bfloat16 [2048, 1024], P('fs', 'tp'), may hold values from -0.5 to 0.5
- second_norm_scale: float32 [2048], replicated, may hold values from 0.1 to 1.9
- mixer_up_matrix: bfloat16 [2048, 4096], P('fs', 'tp'), may hold values from -0.125 to 0.125
- mixer_down_matrix: bfloat16 [2048, 4096], P('fs', 'tp'), may hold values from -0.09375 to 0.09375
Outputs:
- layer_out: bfloat16 [49152, 2048], P(('fs', 'tp'))
The draws below stay inside these ranges and needn't reach their ends.
All inputs are finite; a program needn't handle non-finite values.
Results may differ from the reference program's by a relative error of at most 0.022.
Values may be sent and summed in bfloat16 or wider, within the bound.
No kernel may reach another device: no remote copies, remote signals or barrier semaphores. Data moves between devices by JAX's collectives and lax.ppermute only.
A program may use at most 32 MiB of HBM per device.

```python
import jax
import jax.numpy as jnp
from jax import lax

D = 2048
R_BLOCKS = 16
BLOCK_DIM = 64
RECURRENT_WIDTH = 1024
FF = 4096
TAPS = 4
SEQUENCE_LENGTH = 384
TOKENS = 49152
N_FS = 128
N_TP = 8


def draw_base_decay_logits(key, part):
    pick_key, quick_key, slow_key = jax.random.split(jax.random.fold_in(key, 11), 3)
    quick_share = 0.5
    quick_mask = jax.random.uniform(pick_key, (RECURRENT_WIDTH,), jnp.float32) < quick_share
    quick_speed = jnp.exp(jax.random.uniform(quick_key, (RECURRENT_WIDTH,), jnp.float32, jnp.log(0.004), jnp.log(0.012)))
    slow_speed = jnp.exp(jax.random.uniform(slow_key, (RECURRENT_WIDTH,), jnp.float32, jnp.log(0.03), jnp.log(0.25))) / SEQUENCE_LENGTH
    speeds = jnp.where(quick_mask, quick_speed, slow_speed)
    return (-speeds - jnp.log(-jnp.expm1(-speeds))).astype(jnp.float32)


def draw_extra_log_decay(key, part):
    place_key, depth_key = jax.random.split(jax.random.fold_in(key, 23))
    marked = jax.random.uniform(place_key, (TOKENS, 1), jnp.float32) < 4.0 / SEQUENCE_LENGTH
    kept = jax.random.uniform(depth_key, (TOKENS, RECURRENT_WIDTH), jnp.float32, 0.5, 0.8)
    return jnp.where(marked, jnp.log(kept), 0.0).astype(jnp.float32)


def steps_of(key, shape, shards, smallest, top_value):
    factor_of, own = 1.0, jax.random.fold_in(key, 6)
    for dim, parts in shards:
        steps = jnp.exp(jax.random.uniform(jax.random.fold_in(own, dim), (parts,), jnp.float32, smallest / len(shards), top_value / len(shards)))
        factor_of = factor_of * jnp.repeat(steps, shape[dim] // parts).reshape([-1 if axis == dim else 1 for axis in range(len(shape))])
    return factor_of


def noise(rng, dims, spread, most, shards=(), dtype=jnp.bfloat16):
    values = jax.random.normal(rng, dims, jnp.float32) * spread
    if len(shards) > 0:
        values = steps_of(rng, dims, shards, -0.22, 0.18) * values
    return jnp.clip(values, min=-most, max=most).astype(dtype)


def setup_inputs(seed: int = 0) -> dict:
    keys = jax.random.split(jax.random.key(seed), 14)
    tokens = noise(keys[0], (TOKENS, D), 1.0, 6.0, ((0, 128),))
    first_norm_scale = jnp.clip(1.0 + 0.18 * jax.random.normal(keys[1], (D,), jnp.float32), 0.1, 1.9)
    recurrent_branch_matrix = noise(keys[2], (D, RECURRENT_WIDTH), D ** -0.5, 0.125, ((0, 128), (1, 8)))
    gelu_gate_matrix = noise(keys[3], (D, RECURRENT_WIDTH), D ** -0.5, 0.125, ((0, 128), (1, 8)))
    filter_taps_weight = noise(keys[4], (TAPS, RECURRENT_WIDTH), TAPS ** -0.5, 3.0, ((1, 8),))
    recurrence_gate_blocks = noise(keys[5], (R_BLOCKS, BLOCK_DIM, BLOCK_DIM), BLOCK_DIM ** -0.5, 0.75, ((0, 8),))
    input_gate_blocks = noise(keys[6], (R_BLOCKS, BLOCK_DIM, BLOCK_DIM), BLOCK_DIM ** -0.5, 0.75, ((0, 8),))
    base_decay_logits = draw_base_decay_logits(jax.random.fold_in(keys[13], 71), 0)
    extra_log_decay = draw_extra_log_decay(jax.random.fold_in(keys[13], 71), 0)
    mixer_output_matrix = noise(keys[9], (D, RECURRENT_WIDTH), (RECURRENT_WIDTH // 9) ** -0.5, 0.5, ((0, 128), (1, 8)))
    second_norm_scale = jnp.clip(1.0 + 0.18 * jax.random.normal(keys[10], (D,), jnp.float32), 0.1, 1.9)
    mixer_up_matrix = noise(keys[11], (D, FF), D ** -0.5, 0.125, ((0, 128), (1, 8)))
    mixer_down_matrix = noise(keys[12], (D, FF), FF ** -0.5, 0.09375, ((0, 128), (1, 8)))
    return dict(tokens=tokens, first_norm_scale=first_norm_scale, recurrent_branch_matrix=recurrent_branch_matrix, gelu_gate_matrix=gelu_gate_matrix, filter_taps_weight=filter_taps_weight, recurrence_gate_blocks=recurrence_gate_blocks, input_gate_blocks=input_gate_blocks, base_decay_logits=base_decay_logits, extra_log_decay=extra_log_decay, mixer_output_matrix=mixer_output_matrix, second_norm_scale=second_norm_scale, mixer_up_matrix=mixer_up_matrix, mixer_down_matrix=mixer_down_matrix)


epsilon = 1e-06
decay_rate_scale = 8.0

def rms_scaled(sequence_token_rows, scales):
    widened = sequence_token_rows.astype(jnp.float32)
    mean_square = lax.optimization_barrier(jnp.mean(widened * widened, axis=-1, keepdims=True))
    return (widened * lax.rsqrt(mean_square + epsilon) * scales).astype(jnp.bfloat16)

def linear_combine(earlier, later):
    return (earlier[0] * later[0], later[0] * earlier[1] + later[1])

def causal_taps(branch, filter_taps_weight):
    tap_count = filter_taps_weight.shape[0]
    positions = branch.shape[0]
    padded = jnp.pad(branch.astype(jnp.float32), ((tap_count - 1, 0), (0, 0)))
    running = jnp.zeros(branch.shape, jnp.float32)
    for offset in range(tap_count):
        running = running + padded[offset:offset + positions] * filter_taps_weight[offset].astype(jnp.float32)
    return running.astype(jnp.bfloat16)

def block_map(convolved, blocks):
    positions, channels = convolved.shape
    grouped = convolved.astype(jnp.float32).reshape(positions, blocks.shape[0], blocks.shape[1])
    mapped = jnp.einsum('sgi,gij->sgj', grouped, blocks.astype(jnp.float32))
    return jax.nn.sigmoid(mapped.reshape(positions, channels))

def grouped_sum(left, right, groups):
    width_each = left.shape[1] // groups
    running = jnp.zeros((left.shape[0], right.shape[0]), jnp.float32)
    for column_group in range(groups):
        begin_col = column_group * width_each
        partial_value = jnp.dot(left[:, begin_col:begin_col + width_each], right[:, begin_col:begin_col + width_each].T, preferred_element_type=jnp.float32)
        rounded = lax.optimization_barrier(partial_value.astype(jnp.bfloat16))
        running = running + rounded.astype(jnp.float32)
    return running

def reference(tokens, first_norm_scale, recurrent_branch_matrix, gelu_gate_matrix, filter_taps_weight, recurrence_gate_blocks, input_gate_blocks, base_decay_logits, extra_log_decay, mixer_output_matrix, second_norm_scale, mixer_up_matrix, mixer_down_matrix):

    def single_sequence(input_values):
        sequence_token_rows, extra_decays = input_values
        normed = rms_scaled(sequence_token_rows, first_norm_scale)
        branch = jnp.dot(normed, recurrent_branch_matrix, preferred_element_type=jnp.float32).astype(jnp.bfloat16)
        gate_branch = jnp.dot(normed, gelu_gate_matrix, preferred_element_type=jnp.float32).astype(jnp.bfloat16)
        convolved = causal_taps(branch, filter_taps_weight)
        recurrence_gate_value = block_map(convolved, recurrence_gate_blocks)
        admission = block_map(convolved, input_gate_blocks)
        log_keep_factor = decay_rate_scale * recurrence_gate_value * jax.nn.log_sigmoid(base_decay_logits) + extra_decays
        retain = jnp.exp(log_keep_factor)
        driven = jnp.sqrt(-jnp.expm1(2.0 * log_keep_factor)) * (admission * convolved.astype(jnp.float32))
        memory = lax.associative_scan(linear_combine, (retain, driven), axis=0)[1]
        recurrent = (memory * jax.nn.gelu(gate_branch.astype(jnp.float32))).astype(jnp.bfloat16)
        mixer_out = grouped_sum(recurrent, mixer_output_matrix, N_TP)
        residual = (sequence_token_rows.astype(jnp.float32) + mixer_out).astype(jnp.bfloat16)
        normed_mid = rms_scaled(residual, second_norm_scale)
        raised = jnp.dot(normed_mid, mixer_up_matrix, preferred_element_type=jnp.float32)
        hidden = jnp.square(jax.nn.relu(raised)).astype(jnp.bfloat16)
        channel_sum = grouped_sum(hidden, mixer_down_matrix, N_TP)
        return (residual.astype(jnp.float32) + channel_sum).astype(jnp.bfloat16)
    reshaped_values = tokens.reshape(N_FS, SEQUENCE_LENGTH, D)
    extra_decay_reshaped = extra_log_decay.reshape(N_FS, SEQUENCE_LENGTH, RECURRENT_WIDTH)
    output_values = lax.map(single_sequence, (reshaped_values, extra_decay_reshaped))
    return output_values.reshape(N_FS * SEQUENCE_LENGTH, D)
```

```python
import jax
import jax.numpy as jnp
from jax import lax
from jax.sharding import Mesh, PartitionSpec as P

epsilon = 1e-06
decay_rate_scale = 8.0
wire_scale = 65536.0


def ring(count, step):
    return [(k, (k + step) % count) for k in range(count)]


def rms_scaled(rows, scales):
    widened = rows.astype(jnp.float32)
    mean_square = jnp.mean(widened * widened, axis=-1, keepdims=True)
    return (widened * lax.rsqrt(mean_square + epsilon) * scales).astype(jnp.bfloat16)


def linear_combine(earlier, later):
    return (earlier[0] * later[0], later[0] * earlier[1] + later[1])


def causal_taps(branch, filter_taps_weight):
    tap_count = filter_taps_weight.shape[0]
    positions = branch.shape[0]
    padded = jnp.pad(branch.astype(jnp.float32), ((tap_count - 1, 0), (0, 0)))
    running = jnp.zeros(branch.shape, jnp.float32)
    for offset in range(tap_count):
        running = running + padded[offset : offset + positions] * filter_taps_weight[offset].astype(
            jnp.float32
        )
    return running.astype(jnp.bfloat16)


def block_map(convolved, blocks):
    positions, channels = convolved.shape
    grouped = convolved.reshape(positions, blocks.shape[0], blocks.shape[1])
    mapped = jnp.einsum("sgi,gij->sgj", grouped, blocks, preferred_element_type=jnp.float32)
    return jax.nn.sigmoid(mapped.reshape(positions, channels))


def contract_columns(left, right):
    return lax.dot_general(
        left, right, (((1,), (1,)), ((), ())), preferred_element_type=jnp.float32
    )


def y_pieces(rows):
    count = lax.axis_size("y")
    pieces = [rows]
    for step in (1, count - 1, 2):
        pieces.append(lax.ppermute(rows, "y", ring(count, step)))
    return pieces


def placed(pieces, z_count):
    count = len(pieces)
    height, width = pieces[0].shape
    me = lax.axis_index("y")
    whole = jnp.zeros((z_count, count, height // z_count, width), pieces[0].dtype)
    for step, piece in zip((0, 1, count - 1, 2), pieces):
        origin = lax.rem(me + count - step, count)
        tiles = piece.reshape(z_count, 1, height // z_count, width)
        whole = lax.dynamic_update_slice_in_dim(whole, tiles, origin, 1)
    return whole.reshape(count * height, width)


def x_summed(rows):
    count = lax.axis_size("x")
    tiles = rows.reshape(count, rows.shape[0] // count, rows.shape[1])
    arrived = lax.all_to_all(tiles, "x", 0, 0, tiled=True)
    return arrived.astype(jnp.float32).sum(axis=0)


def added(left, right):
    return (left.astype(jnp.float32) + right.astype(jnp.float32)).astype(jnp.bfloat16)


def layer(
    tokens,
    first_norm_scale,
    recurrent_branch_matrix,
    gelu_gate_matrix,
    filter_taps_weight,
    recurrence_gate_blocks,
    input_gate_blocks,
    base_decay_logits,
    extra_log_decay,
    mixer_output_matrix,
    second_norm_scale,
    mixer_up_matrix,
    mixer_down_matrix,
):
    positions, _ = tokens.shape
    z_count, x_count, c_count = (lax.axis_size(k) for k in ("z", "x", "c"))
    own_count = positions // (x_count * c_count)
    x_index, c_index = lax.axis_index("x"), lax.axis_index("c")
    channels = recurrent_branch_matrix.shape[1]

    shards = jnp.concatenate(
        [
            recurrent_branch_matrix,
            gelu_gate_matrix,
            mixer_output_matrix,
            mixer_up_matrix,
            mixer_down_matrix,
        ],
        axis=1,
    )
    sent = (shards.astype(jnp.float32) * wire_scale).astype(jnp.float16)
    z_rows = lax.all_gather(sent, "z", axis=0, tiled=True)
    z_rows = (z_rows.astype(jnp.float32) * (1.0 / wire_scale)).astype(jnp.bfloat16)
    first_pieces = y_pieces(z_rows[:, : 3 * channels])
    second_pieces = y_pieces(z_rows[:, 3 * channels :])
    first = placed(first_pieces, z_count)
    second = placed(second_pieces, z_count)
    branch_full, gate_full, out_full = jnp.split(first, 3, axis=1)
    up_full, down_full = jnp.split(second, 2, axis=1)

    normed = rms_scaled(tokens, first_norm_scale)
    branch = jnp.dot(normed, branch_full, preferred_element_type=jnp.float32).astype(jnp.bfloat16)
    gate_branch = jnp.dot(normed, gate_full, preferred_element_type=jnp.float32).astype(
        jnp.bfloat16
    )
    convolved = causal_taps(branch, filter_taps_weight)
    rate = block_map(convolved, recurrence_gate_blocks)
    admission = block_map(convolved, input_gate_blocks)
    log_keep = decay_rate_scale * rate * jax.nn.log_sigmoid(base_decay_logits) + extra_log_decay
    retain = jnp.exp(log_keep)
    driven = jnp.sqrt(-jnp.expm1(2.0 * log_keep)) * (admission * convolved.astype(jnp.float32))
    memory = lax.associative_scan(linear_combine, (retain, driven), axis=0)[1]
    recurrent = (memory * jax.nn.gelu(gate_branch.astype(jnp.float32))).astype(jnp.bfloat16)

    by_core = recurrent.reshape(x_count, c_count, own_count, channels)

    def rows_of(core):
        return lax.dynamic_index_in_dim(by_core, core, 1, keepdims=False).reshape(-1, channels)

    given = contract_columns(rows_of(1 - c_index), out_full).astype(jnp.bfloat16)
    kept = contract_columns(rows_of(c_index), out_full).astype(jnp.bfloat16)
    mixer_out = x_summed(added(kept, lax.ppermute(given, "c", ring(c_count, 1))))
    own_rows = lax.dynamic_slice_in_dim(
        tokens, (x_index * c_count + c_index) * own_count, own_count, 0
    )
    residual = (own_rows.astype(jnp.float32) + mixer_out).astype(jnp.bfloat16)
    normed_mid = rms_scaled(residual, second_norm_scale)

    mine = lax.all_gather(normed_mid, "x", axis=0, tiled=True)
    other = lax.ppermute(mine, "c", ring(c_count, 1))

    def mixed(rows):
        raised = jnp.dot(rows, up_full, preferred_element_type=jnp.float32)
        hidden = jnp.square(jax.nn.relu(raised)).astype(jnp.bfloat16)
        return contract_columns(hidden, down_full).astype(jnp.bfloat16)

    given = mixed(other)
    kept = mixed(mine)
    channel_sum = x_summed(added(kept, lax.ppermute(given, "c", ring(c_count, 1))))
    return (residual.astype(jnp.float32) + channel_sum).astype(jnp.bfloat16)


def solution(mesh):
    z_count = 32 if mesh.shape["fs"] == 128 else mesh.shape["fs"] // 4
    split = Mesh(
        mesh.devices.reshape(z_count, mesh.shape["fs"] // z_count, mesh.shape["tp"] // 2, 2),
        ("z", "y", "x", "c"),
    )
    fs, tp = ("z", "y"), ("x", "c")
    in_specs = (
        P(fs, None),
        P(),
        P(fs, tp),
        P(fs, tp),
        P(None, tp),
        P(tp, None, None),
        P(tp, None, None),
        P(tp),
        P(fs, tp),
        P(fs, tp),
        P(),
        P(fs, tp),
        P(fs, tp),
    )
    return jax.shard_map(
        layer, mesh=split, in_specs=in_specs, out_specs=P((*fs, *tp), None), check_vma=False
    )
```

```python
import jax
import jax.numpy as jnp
from jax import lax
from jax.experimental import pallas as pl
from jax.experimental.pallas import tpu as pltpu
from jax.sharding import Mesh, PartitionSpec as P


epsilon = 1e-06
decay_rate_scale = 8.0
wire_scale = 65536.0
row_scale = 512.0


def ring(count, step):
    return [(k, (k + step) % count) for k in range(count)]


def rms_scaled(rows, scales):
    widened = rows.astype(jnp.float32)
    mean_square = jnp.mean(widened * widened, axis=-1, keepdims=True)
    return (widened * lax.rsqrt(mean_square + epsilon) * scales).astype(jnp.bfloat16)


def shifted(rows, step, fill):
    index = lax.broadcasted_iota(jnp.int32, rows.shape, 0)
    return jnp.where(index >= step, pltpu.roll(rows, step, 0), fill)


def one_minus_exp(value):
    terms = 1.0 + value * (1.0 / 8.0)
    for order in (7.0, 6.0, 5.0, 4.0, 3.0, 2.0):
        terms = 1.0 + value * (1.0 / order) * terms
    return jnp.where(value > -0.3, -value * terms, 1.0 - jnp.exp(value))


def assemble(pieces, whole):
    me = lax.axis_index("y")
    for step, piece in zip((0, 1, 3, 2), pieces):
        whole[:, lax.rem(me + 4 - step, 4)] = piece[...]


def join_kernel(a_ref, b_ref, c_ref, d_ref, e_ref, out_ref):
    begin = 0
    for ref in (a_ref, b_ref, c_ref, d_ref, e_ref):
        stop = begin + ref.shape[1]
        out_ref[:, begin:stop] = ref[...] * jnp.asarray(wire_scale, ref.dtype)
        begin = stop


def mixer_kernel(
    normed, taps, gates, decay, extra, p0, p1, p2, p3, given, kept, whole, kept_rows
):
    positions, channels = extra.shape
    core = lax.axis_index("c")
    assemble((p0, p1, p2, p3), whole)
    weights = whole[...].reshape(normed.shape[1], 3 * channels)
    both = jnp.dot(
        normed[...], weights[:, : 2 * channels], preferred_element_type=jnp.float32
    )
    branch = both[:, :channels].astype(jnp.bfloat16).astype(jnp.float32)
    gate = both[:, channels:].astype(jnp.bfloat16).astype(jnp.float32)
    tap = taps[...].astype(jnp.float32)
    running = branch * tap[3:4]
    for back in (1, 2, 3):
        running = running + shifted(branch, back, 0.0) * tap[3 - back : 4 - back]
    convolved = running.astype(jnp.bfloat16)
    mapped = jax.nn.sigmoid(
        jnp.dot(convolved, gates[...], preferred_element_type=jnp.float32)
    )
    log_keep = mapped[:, :channels] * decay[...] + extra[...]
    retain = jnp.exp(log_keep)
    memory = jnp.sqrt(one_minus_exp(2.0 * log_keep)) * (
        mapped[:, channels:] * convolved.astype(jnp.float32)
    )
    step = 1
    while step < positions:
        memory = retain * shifted(memory, step, 0.0) + memory
        retain = retain * shifted(retain, step, 1.0)
        step *= 2
    inner = 0.7978845608028654 * (gate + 0.044715 * gate * gate * gate)
    recurrent = (memory * (0.5 * gate * (1.0 + jnp.tanh(inner)))).astype(jnp.bfloat16)
    kept_rows[...] = recurrent.reshape(kept_rows.shape)
    out_rows = weights[:, 2 * channels :]
    for ref, which in ((given, 1 - core), (kept, core)):
        rows = kept_rows[:, which].reshape(positions // 2, channels)
        ref[...] = contract_columns(rows, out_rows).astype(jnp.bfloat16)


def channel_kernel(rows, p0, p1, p2, p3, given, kept, whole, hidden_rows):
    positions, width = rows.shape
    core = lax.axis_index("c")
    assemble((p0, p1, p2, p3), whole)
    half = whole.shape[3] // 2
    weights = whole[...].reshape(width, 2 * half)
    raised = jnp.dot(rows[...], weights[:, :half], preferred_element_type=jnp.float32)
    hidden = jnp.square(jnp.maximum(raised, 0.0)).astype(jnp.bfloat16)
    hidden_rows[...] = hidden.reshape(hidden_rows.shape)
    for ref, which in ((given, 1 - core), (kept, core)):
        picked = hidden_rows[:, which].reshape(positions // 2, half)
        ref[...] = contract_columns(picked, weights[:, half:]).astype(jnp.bfloat16)


def contract_columns(left, right):
    return lax.dot_general(
        left, right, (((1,), (1,)), ((), ())), preferred_element_type=jnp.float32
    )


def in_vmem(count):
    return [pl.BlockSpec(memory_space=pltpu.VMEM)] * count


def mixed(kernel, operands, pieces, scratch_rows, flops):
    z_count, height, columns = pieces[0].shape
    half = jax.ShapeDtypeStruct((operands[0].shape[0] // 2, operands[0].shape[1]), jnp.bfloat16)
    return pl.pallas_call(
        kernel,
        out_shape=(half, half),
        in_specs=in_vmem(len(operands) + len(pieces)),
        out_specs=tuple(in_vmem(2)),
        scratch_shapes=[
            pltpu.VMEM((z_count, len(pieces), height, columns), jnp.bfloat16),
            pltpu.VMEM(scratch_rows, jnp.bfloat16),
        ],
        compiler_params=pltpu.CompilerParams(vmem_limit_bytes=24 << 20),
        cost_estimate=pl.CostEstimate(flops=flops, bytes_accessed=8 << 20, transcendentals=0),
    )(*operands, *pieces)


def y_pieces(rows, height):
    count = lax.axis_size("y")
    pieces = [rows]
    for step in (1, count - 1, 2):
        pieces.append(lax.ppermute(rows, "y", ring(count, step)))
    return [piece.reshape(-1, height, rows.shape[1]) for piece in pieces]


def x_summed(rows):
    count = lax.axis_size("x")
    tiles = rows.reshape(count, rows.shape[0] // count, rows.shape[1])
    arrived = lax.all_to_all(tiles, "x", 0, 0, tiled=True)
    return arrived.astype(jnp.float32).sum(axis=0)


def added(left, right):
    return (left.astype(jnp.float32) + right.astype(jnp.float32)).astype(jnp.bfloat16)


def layer(
    tokens,
    first_norm_scale,
    recurrent_branch_matrix,
    gelu_gate_matrix,
    filter_taps_weight,
    recurrence_gate_blocks,
    input_gate_blocks,
    base_decay_logits,
    extra_log_decay,
    mixer_output_matrix,
    second_norm_scale,
    mixer_up_matrix,
    mixer_down_matrix,
):
    positions, width = tokens.shape
    _, x_count, c_count = (lax.axis_size(k) for k in ("z", "x", "c"))
    own_count = positions // (x_count * c_count)
    x_index, c_index = lax.axis_index("x"), lax.axis_index("c")
    channels = recurrent_branch_matrix.shape[1]

    height = recurrent_branch_matrix.shape[0]
    matrices = (
        recurrent_branch_matrix,
        gelu_gate_matrix,
        mixer_output_matrix,
        mixer_up_matrix,
        mixer_down_matrix,
    )
    joined = pl.pallas_call(
        join_kernel,
        out_shape=jax.ShapeDtypeStruct((height, sum(k.shape[1] for k in matrices)), jnp.bfloat16),
        in_specs=in_vmem(len(matrices)),
        out_specs=in_vmem(1)[0],
        name="join",
    )(*matrices)
    z_rows = lax.all_gather(joined.astype(jnp.float16), "z", axis=0, tiled=True)
    z_rows = (z_rows.astype(jnp.float32) * (1.0 / wire_scale)).astype(jnp.bfloat16)
    first = y_pieces(z_rows[:, : 3 * channels], height)
    second = y_pieces(z_rows[:, 3 * channels :], height)

    normed = rms_scaled(tokens, first_norm_scale)
    diagonal = jnp.zeros((2, channels // 2, 2, 2, channels // 2), jnp.bfloat16)
    for group in range(2):
        diagonal = diagonal.at[group, :, 0, group].set(recurrence_gate_blocks[group])
        diagonal = diagonal.at[group, :, 1, group].set(input_gate_blocks[group])
    decay = (decay_rate_scale * jax.nn.log_sigmoid(base_decay_logits))[None]

    def given_summed(given, kept):
        return x_summed(added(kept, lax.ppermute(given, "c", ring(c_count, 1))))

    by_core = (x_count, c_count, own_count)
    given, kept = mixed(
        mixer_kernel,
        (normed, filter_taps_weight, diagonal.reshape(channels, -1), decay, extra_log_decay),
        first,
        (*by_core, channels),
        6 * positions * width * channels,
    )
    mixer_out = given_summed(given, kept)
    own_rows = lax.dynamic_slice_in_dim(
        tokens, (x_index * c_count + c_index) * own_count, own_count, 0
    )
    residual = (own_rows.astype(jnp.float32) + mixer_out).astype(jnp.bfloat16)
    normed_mid = rms_scaled(residual, second_norm_scale)
    sent = (normed_mid.astype(jnp.float32) * row_scale).astype(jnp.float16)
    arrived = lax.all_gather(sent, ("x", "c"), axis=0, tiled=True)
    rows = (arrived.astype(jnp.float32) * (1.0 / row_scale)).astype(jnp.bfloat16)
    given, kept = mixed(
        channel_kernel,
        (rows,),
        second,
        (*by_core, mixer_up_matrix.shape[1]),
        4 * positions * width * mixer_up_matrix.shape[1],
    )
    channel_sum = given_summed(given, kept)
    return (residual.astype(jnp.float32) + channel_sum).astype(jnp.bfloat16)


def solution(mesh):
    z_count = 32 if mesh.shape["fs"] == 128 else mesh.shape["fs"] // 4
    split = Mesh(
        mesh.devices.reshape(z_count, mesh.shape["fs"] // z_count, mesh.shape["tp"] // 2, 2),
        ("z", "y", "x", "c"),
    )
    fs, tp = ("z", "y"), ("x", "c")
    in_specs = (
        P(fs, None),
        P(),
        P(fs, tp),
        P(fs, tp),
        P(None, tp),
        P(tp, None, None),
        P(tp, None, None),
        P(tp),
        P(fs, tp),
        P(fs, tp),
        P(),
        P(fs, tp),
        P(fs, tp),
    )
    return jax.shard_map(
        layer, mesh=split, in_specs=in_specs, out_specs=P((*fs, *tp), None), check_vma=False
    )
```

```python
import jax
import jax.numpy as jnp
from jax import lax
from jax.experimental import pallas as pl
from jax.experimental.pallas import tpu as pltpu
from jax.sharding import Mesh, PartitionSpec as P


epsilon = 1e-06
decay_rate_scale = 8.0
wire_scale = 65536.0
row_scale = 512.0
narrow_steps = (2, 1, 3)
wide_steps = (1, 3, 2)


def ring(count, step):
    return [(k, (k + step) % count) for k in range(count)]


def rms_scaled(rows, scales):
    widened = rows.astype(jnp.float32)
    mean_square = jnp.mean(widened * widened, axis=-1, keepdims=True)
    return (widened * lax.rsqrt(mean_square + epsilon) * scales).astype(jnp.bfloat16)


def shifted(rows, step, fill):
    index = lax.broadcasted_iota(jnp.int32, rows.shape, 0)
    return jnp.where(index >= step, pltpu.roll(rows, step, 0), fill)


def one_minus_exp(value):
    terms = 1.0 + value * (1.0 / 8.0)
    for order in (7.0, 6.0, 5.0, 4.0, 3.0, 2.0):
        terms = 1.0 + value * (1.0 / order) * terms
    return jnp.where(value > -0.3, -value * terms, 1.0 - jnp.exp(value))


def assemble(pieces, whole):
    me = lax.axis_index("y")
    for step, piece in enumerate(pieces):
        whole[:, lax.rem(me + 4 - step, 4)] = piece[...]


def join_kernel(a_ref, b_ref, c_ref, d_ref, e_ref, out_ref):
    begin = 0
    for ref in (a_ref, b_ref, c_ref, d_ref, e_ref):
        stop = begin + ref.shape[1]
        out_ref[:, begin:stop] = ref[...] * jnp.asarray(wire_scale, ref.dtype)
        begin = stop


def mixer_kernel(
    normed, taps, gates, decay, extra, p0, p1, p2, p3, given, kept, whole, kept_rows
):
    positions, channels = extra.shape
    core = lax.axis_index("c")
    assemble((p0, p1, p2, p3), whole)
    weights = whole[...].reshape(normed.shape[1], 3 * channels)
    both = jnp.dot(
        normed[...], weights[:, : 2 * channels], preferred_element_type=jnp.float32
    )
    branch = both[:, :channels].astype(jnp.bfloat16).astype(jnp.float32)
    gate = both[:, channels:].astype(jnp.bfloat16).astype(jnp.float32)
    tap = taps[...].astype(jnp.float32)
    running = branch * tap[3:4]
    for back in (1, 2, 3):
        running = running + shifted(branch, back, 0.0) * tap[3 - back : 4 - back]
    convolved = running.astype(jnp.bfloat16)
    mapped = jax.nn.sigmoid(
        jnp.dot(convolved, gates[...], preferred_element_type=jnp.float32)
    )
    log_keep = mapped[:, :channels] * decay[...] + extra[...]
    retain = jnp.exp(log_keep)
    memory = jnp.sqrt(one_minus_exp(2.0 * log_keep)) * (
        mapped[:, channels:] * convolved.astype(jnp.float32)
    )
    step = 1
    while step < positions:
        memory = retain * shifted(memory, step, 0.0) + memory
        retain = retain * shifted(retain, step, 1.0)
        step *= 2
    inner = 0.7978845608028654 * (gate + 0.044715 * gate * gate * gate)
    recurrent = (memory * (0.5 * gate * (1.0 + jnp.tanh(inner)))).astype(jnp.bfloat16)
    kept_rows[...] = recurrent.reshape(kept_rows.shape)
    out_rows = weights[:, 2 * channels :]
    for ref, which in ((given, 1 - core), (kept, core)):
        rows = kept_rows[:, which].reshape(positions // 2, channels)
        ref[...] = contract_columns(rows, out_rows).astype(jnp.bfloat16)


def channel_kernel(rows, p0, p1, p2, p3, given, kept, whole, hidden_rows):
    positions, width = rows.shape
    core = lax.axis_index("c")
    assemble((p0, p1, p2, p3), whole)
    half = whole.shape[3] // 2
    weights = whole[...].reshape(width, 2 * half)
    raised = jnp.dot(rows[...], weights[:, :half], preferred_element_type=jnp.float32)
    hidden = jnp.square(jnp.maximum(raised, 0.0)).astype(jnp.bfloat16)
    hidden_rows[...] = hidden.reshape(hidden_rows.shape)
    for ref, which in ((given, 1 - core), (kept, core)):
        picked = hidden_rows[:, which].reshape(positions // 2, half)
        ref[...] = contract_columns(picked, weights[:, half:]).astype(jnp.bfloat16)


def contract_columns(left, right):
    return lax.dot_general(
        left, right, (((1,), (1,)), ((), ())), preferred_element_type=jnp.float32
    )


def in_vmem(count):
    return [pl.BlockSpec(memory_space=pltpu.VMEM)] * count


def mixed(kernel, operands, pieces, scratch_rows, flops):
    z_count, height, columns = pieces[0].shape
    half = jax.ShapeDtypeStruct((operands[0].shape[0] // 2, operands[0].shape[1]), jnp.bfloat16)
    return pl.pallas_call(
        kernel,
        out_shape=(half, half),
        in_specs=in_vmem(len(operands) + len(pieces)),
        out_specs=tuple(in_vmem(2)),
        scratch_shapes=[
            pltpu.VMEM((z_count, len(pieces), height, columns), jnp.bfloat16),
            pltpu.VMEM(scratch_rows, jnp.bfloat16),
        ],
        compiler_params=pltpu.CompilerParams(vmem_limit_bytes=24 << 20),
        cost_estimate=pl.CostEstimate(flops=flops, bytes_accessed=8 << 20, transcendentals=0),
    )(*operands, *pieces)


def y_pieces(rows, steps, height):
    pieces = {0: rows}
    for step in steps:
        pieces[step] = lax.ppermute(rows, "y", ring(lax.axis_size("y"), step))
    return [pieces[k].reshape(-1, height, rows.shape[1]) for k in range(len(pieces))]


def x_spread(rows):
    count = lax.axis_size("x")
    tiles = rows.reshape(count, rows.shape[0] // count, rows.shape[1])
    return lax.all_to_all(tiles, "x", 0, 0, tiled=True)


def settle_kernel(arrived, own_rows, scale, residual, sent):
    total = arrived[0].astype(jnp.float32)
    for k in range(1, arrived.shape[0]):
        total = total + arrived[k].astype(jnp.float32)
    rows = (own_rows[...].astype(jnp.float32) + total).astype(jnp.bfloat16)
    residual[...] = rows
    sent[...] = rms_scaled(rows, scale[...]) * jnp.asarray(row_scale, jnp.bfloat16)


def added(left, right):
    return (left.astype(jnp.float32) + right.astype(jnp.float32)).astype(jnp.bfloat16)


def layer(
    tokens,
    first_norm_scale,
    recurrent_branch_matrix,
    gelu_gate_matrix,
    filter_taps_weight,
    recurrence_gate_blocks,
    input_gate_blocks,
    base_decay_logits,
    extra_log_decay,
    mixer_output_matrix,
    second_norm_scale,
    mixer_up_matrix,
    mixer_down_matrix,
):
    positions, width = tokens.shape
    _, x_count, c_count = (lax.axis_size(k) for k in ("z", "x", "c"))
    own_count = positions // (x_count * c_count)
    x_index, c_index = lax.axis_index("x"), lax.axis_index("c")
    channels = recurrent_branch_matrix.shape[1]

    height = recurrent_branch_matrix.shape[0]
    matrices = (
        recurrent_branch_matrix,
        gelu_gate_matrix,
        mixer_output_matrix,
        mixer_up_matrix,
        mixer_down_matrix,
    )
    joined = pl.pallas_call(
        join_kernel,
        out_shape=jax.ShapeDtypeStruct((height, sum(k.shape[1] for k in matrices)), jnp.bfloat16),
        in_specs=in_vmem(len(matrices)),
        out_specs=in_vmem(1)[0],
        compiler_params=pltpu.CompilerParams(vmem_limit_bytes=4 << 20),
        name="join",
    )(*matrices)
    z_rows = lax.all_gather(joined.astype(jnp.float16), "z", axis=0, tiled=True)
    z_rows = (z_rows.astype(jnp.float32) * (1.0 / wire_scale)).astype(jnp.bfloat16)
    first = y_pieces(z_rows[:, : 3 * channels], narrow_steps, height)
    second = y_pieces(z_rows[:, 3 * channels :], wide_steps, height)

    normed = rms_scaled(tokens, first_norm_scale)
    own_rows = lax.dynamic_slice_in_dim(
        tokens, (x_index * c_count + c_index) * own_count, own_count, 0
    )
    normed, own_rows = lax.optimization_barrier((normed, own_rows))
    diagonal = jnp.zeros((2, channels // 2, 2, 2, channels // 2), jnp.bfloat16)
    for group in range(2):
        diagonal = diagonal.at[group, :, 0, group].set(recurrence_gate_blocks[group])
        diagonal = diagonal.at[group, :, 1, group].set(input_gate_blocks[group])
    decay = (decay_rate_scale * jax.nn.log_sigmoid(base_decay_logits))[None]

    def exchanged(given, kept):
        return x_spread(added(kept, lax.ppermute(given, "c", ring(c_count, 1))))

    by_core = (x_count, c_count, own_count)
    given, kept = mixed(
        mixer_kernel,
        (normed, filter_taps_weight, diagonal.reshape(channels, -1), decay, extra_log_decay),
        first,
        (*by_core, channels),
        6 * positions * width * channels,
    )
    rows_out = jax.ShapeDtypeStruct((own_count, width), jnp.bfloat16)
    residual, sent = pl.pallas_call(
        settle_kernel,
        out_shape=(rows_out, rows_out),
        in_specs=in_vmem(3),
        out_specs=tuple(in_vmem(2)),
        compiler_params=pltpu.CompilerParams(vmem_limit_bytes=8 << 20),
        name="settle",
    )(exchanged(given, kept), own_rows, second_norm_scale[None])
    sent = sent.astype(jnp.float16)
    arrived = lax.all_gather(sent, ("x", "c"), axis=0, tiled=True)
    rows = (arrived.astype(jnp.float32) * (1.0 / row_scale)).astype(jnp.bfloat16)
    given, kept = mixed(
        channel_kernel,
        (rows,),
        second,
        (*by_core, mixer_up_matrix.shape[1]),
        4 * positions * width * mixer_up_matrix.shape[1],
    )
    channel_sum = exchanged(given, kept).astype(jnp.float32).sum(axis=0)
    return (residual.astype(jnp.float32) + channel_sum).astype(jnp.bfloat16)


def solution(mesh):
    z_count = 32 if mesh.shape["fs"] == 128 else mesh.shape["fs"] // 4
    split = Mesh(
        mesh.devices.reshape(z_count, mesh.shape["fs"] // z_count, mesh.shape["tp"] // 2, 2),
        ("z", "y", "x", "c"),
    )
    fs, tp = ("z", "y"), ("x", "c")
    in_specs = (
        P(fs, None),
        P(),
        P(fs, tp),
        P(fs, tp),
        P(None, tp),
        P(tp, None, None),
        P(tp, None, None),
        P(tp),
        P(fs, tp),
        P(fs, tp),
        P(),
        P(fs, tp),
        P(fs, tp),
    )
    return jax.shard_map(
        layer, mesh=split, in_specs=in_specs, out_specs=P((*fs, *tp), None), check_vma=False
    )
```

```python
import jax
import jax.numpy as jnp
from jax import lax
from jax.experimental import pallas as pl
from jax.experimental.pallas import tpu as pltpu
from jax.sharding import Mesh, PartitionSpec as P


epsilon = 1e-06
decay_rate_scale = 8.0
wire_scale = 65536.0
row_scale = 512.0
narrow_steps = (2, 3, 1)
wide_steps = (3, 1, 2)


def ring(count, step):
    return [(k, (k + step) % count) for k in range(count)]


def rms_scaled(rows, scales):
    widened = rows.astype(jnp.float32)
    mean_square = jnp.mean(widened * widened, axis=-1, keepdims=True)
    return (widened * lax.rsqrt(mean_square + epsilon) * scales).astype(jnp.bfloat16)


def shifted(rows, step, fill):
    index = lax.broadcasted_iota(jnp.int32, rows.shape, 0)
    return jnp.where(index >= step, pltpu.roll(rows, step, 0), fill)


def one_minus_exp(value):
    terms = 1.0 + value * (1.0 / 8.0)
    for order in (7.0, 6.0, 5.0, 4.0, 3.0, 2.0):
        terms = 1.0 + value * (1.0 / order) * terms
    return jnp.where(value > -0.3, -value * terms, 1.0 - jnp.exp(value))


def assemble(pieces, whole):
    me = lax.axis_index("y")
    for step, piece in enumerate(pieces):
        whole[:, lax.rem(me + 4 - step, 4)] = piece[...]


def join_kernel(a_ref, b_ref, c_ref, d_ref, e_ref, out_ref):
    begin = 0
    for ref in (a_ref, b_ref, c_ref, d_ref, e_ref):
        stop = begin + ref.shape[1]
        out_ref[:, begin:stop] = ref[...] * jnp.asarray(wire_scale, ref.dtype)
        begin = stop


def mixer_kernel(
    normed, taps, gates, decay, extra, p0, p1, p2, p3, given, kept, whole, kept_rows
):
    positions, channels = extra.shape
    core = lax.axis_index("c")
    assemble((p0, p1, p2, p3), whole)
    weights = whole[...].reshape(normed.shape[1], 3 * channels)
    both = jnp.dot(
        normed[...], weights[:, : 2 * channels], preferred_element_type=jnp.float32
    )
    branch = both[:, :channels].astype(jnp.bfloat16).astype(jnp.float32)
    gate = both[:, channels:].astype(jnp.bfloat16).astype(jnp.float32)
    tap = taps[...].astype(jnp.float32)
    running = branch * tap[3:4]
    for back in (1, 2, 3):
        running = running + shifted(branch, back, 0.0) * tap[3 - back : 4 - back]
    convolved = running.astype(jnp.bfloat16)
    mapped = jax.nn.sigmoid(
        jnp.dot(convolved, gates[...], preferred_element_type=jnp.float32)
    )
    log_keep = mapped[:, :channels] * decay[...] + extra[...]
    retain = jnp.exp(log_keep)
    memory = jnp.sqrt(one_minus_exp(2.0 * log_keep)) * (
        mapped[:, channels:] * convolved.astype(jnp.float32)
    )
    step = 1
    while step < positions:
        memory = retain * shifted(memory, step, 0.0) + memory
        retain = retain * shifted(retain, step, 1.0)
        step *= 2
    inner = 0.7978845608028654 * (gate + 0.044715 * gate * gate * gate)
    recurrent = (memory * (0.5 * gate * (1.0 + jnp.tanh(inner)))).astype(jnp.bfloat16)
    kept_rows[...] = recurrent.reshape(kept_rows.shape)
    out_rows = weights[:, 2 * channels :]
    for ref, which in ((given, 1 - core), (kept, core)):
        rows = kept_rows[:, which].reshape(positions // 2, channels)
        ref[...] = contract_columns(rows, out_rows).astype(jnp.bfloat16)


def channel_kernel(rows, p0, p1, p2, p3, given, kept, whole, hidden_rows):
    positions, width = rows.shape
    core = lax.axis_index("c")
    assemble((p0, p1, p2, p3), whole)
    half = whole.shape[3] // 2
    weights = whole[...].reshape(width, 2 * half)
    raised = jnp.dot(rows[...], weights[:, :half], preferred_element_type=jnp.float32)
    hidden = jnp.square(jnp.maximum(raised, 0.0)).astype(jnp.bfloat16)
    hidden_rows[...] = hidden.reshape(hidden_rows.shape)
    for ref, which in ((given, 1 - core), (kept, core)):
        picked = hidden_rows[:, which].reshape(positions // 2, half)
        ref[...] = contract_columns(picked, weights[:, half:]).astype(jnp.bfloat16)


def contract_columns(left, right):
    return lax.dot_general(
        left, right, (((1,), (1,)), ((), ())), preferred_element_type=jnp.float32
    )


def in_vmem(count):
    return [pl.BlockSpec(memory_space=pltpu.VMEM)] * count


def mixed(kernel, operands, pieces, scratch_rows, flops):
    z_count, height, columns = pieces[0].shape
    half = jax.ShapeDtypeStruct((operands[0].shape[0] // 2, operands[0].shape[1]), jnp.bfloat16)
    return pl.pallas_call(
        kernel,
        out_shape=(half, half),
        in_specs=in_vmem(len(operands) + len(pieces)),
        out_specs=tuple(in_vmem(2)),
        scratch_shapes=[
            pltpu.VMEM((z_count, len(pieces), height, columns), jnp.bfloat16),
            pltpu.VMEM(scratch_rows, jnp.bfloat16),
        ],
        compiler_params=pltpu.CompilerParams(vmem_limit_bytes=24 << 20),
        cost_estimate=pl.CostEstimate(flops=flops, bytes_accessed=8 << 20, transcendentals=0),
    )(*operands, *pieces)


def y_pieces(rows, steps, height):
    pieces = {0: rows}
    for step in steps:
        pieces[step] = lax.ppermute(rows, "y", ring(lax.axis_size("y"), step))
    return [pieces[k].reshape(-1, height, rows.shape[1]) for k in range(len(pieces))]


def x_spread(rows):
    count = lax.axis_size("x")
    tiles = rows.reshape(count, rows.shape[0] // count, rows.shape[1])
    return lax.all_to_all(tiles, "x", 0, 0, tiled=True)


def settle_kernel(arrived, own_rows, scale, residual, sent):
    total = arrived[0].astype(jnp.float32)
    for k in range(1, arrived.shape[0]):
        total = total + arrived[k].astype(jnp.float32)
    rows = (own_rows[...].astype(jnp.float32) + total).astype(jnp.bfloat16)
    residual[...] = rows
    sent[...] = rms_scaled(rows, scale[...]) * jnp.asarray(row_scale, jnp.bfloat16)


def added(left, right):
    return (left.astype(jnp.float32) + right.astype(jnp.float32)).astype(jnp.bfloat16)


def layer(
    tokens,
    first_norm_scale,
    recurrent_branch_matrix,
    gelu_gate_matrix,
    filter_taps_weight,
    recurrence_gate_blocks,
    input_gate_blocks,
    base_decay_logits,
    extra_log_decay,
    mixer_output_matrix,
    second_norm_scale,
    mixer_up_matrix,
    mixer_down_matrix,
):
    positions, width = tokens.shape
    _, x_count, c_count = (lax.axis_size(k) for k in ("z", "x", "c"))
    own_count = positions // (x_count * c_count)
    x_index, c_index = lax.axis_index("x"), lax.axis_index("c")
    channels = recurrent_branch_matrix.shape[1]

    height = recurrent_branch_matrix.shape[0]
    matrices = (
        recurrent_branch_matrix,
        gelu_gate_matrix,
        mixer_output_matrix,
        mixer_up_matrix,
        mixer_down_matrix,
    )
    joined = pl.pallas_call(
        join_kernel,
        out_shape=jax.ShapeDtypeStruct((height, sum(k.shape[1] for k in matrices)), jnp.bfloat16),
        in_specs=in_vmem(len(matrices)),
        out_specs=in_vmem(1)[0],
        name="join",
    )(*matrices)
    z_rows = lax.all_gather(joined.astype(jnp.float16), "z", axis=0, tiled=True)
    z_rows = (z_rows.astype(jnp.float32) * (1.0 / wire_scale)).astype(jnp.bfloat16)
    first = y_pieces(z_rows[:, : 3 * channels], narrow_steps, height)
    second = y_pieces(z_rows[:, 3 * channels :], wide_steps, height)

    normed = rms_scaled(tokens, first_norm_scale)
    own_rows = lax.dynamic_slice_in_dim(
        tokens, (x_index * c_count + c_index) * own_count, own_count, 0
    )
    normed, own_rows = lax.optimization_barrier((normed, own_rows))
    diagonal = jnp.zeros((2, channels // 2, 2, 2, channels // 2), jnp.bfloat16)
    for group in range(2):
        diagonal = diagonal.at[group, :, 0, group].set(recurrence_gate_blocks[group])
        diagonal = diagonal.at[group, :, 1, group].set(input_gate_blocks[group])
    decay = (decay_rate_scale * jax.nn.log_sigmoid(base_decay_logits))[None]

    def exchanged(given, kept):
        taken = lax.ppermute(given, "c", ring(c_count, 1))
        both = added(kept, taken)
        return x_spread(both)

    by_core = (x_count, c_count, own_count)
    given, kept = mixed(
        mixer_kernel,
        (normed, filter_taps_weight, diagonal.reshape(channels, -1), decay, extra_log_decay),
        first,
        (*by_core, channels),
        6 * positions * width * channels,
    )
    rows_out = jax.ShapeDtypeStruct((own_count, width), jnp.bfloat16)
    residual, sent = pl.pallas_call(
        settle_kernel,
        out_shape=(rows_out, rows_out),
        in_specs=in_vmem(3),
        out_specs=tuple(in_vmem(2)),
        compiler_params=pltpu.CompilerParams(vmem_limit_bytes=8 << 20),
        name="settle",
    )(exchanged(given, kept), own_rows, second_norm_scale[None])
    sent = sent.astype(jnp.float16)
    arrived = lax.all_gather(sent, ("x", "c"), axis=0, tiled=True)
    rows = (arrived.astype(jnp.float32) * (1.0 / row_scale)).astype(jnp.bfloat16)
    given, kept = mixed(
        channel_kernel,
        (rows,),
        second,
        (*by_core, mixer_up_matrix.shape[1]),
        4 * positions * width * mixer_up_matrix.shape[1],
    )
    channel_sum = exchanged(given, kept).astype(jnp.float32).sum(axis=0)
    return (residual.astype(jnp.float32) + channel_sum).astype(jnp.bfloat16)


def solution(mesh):
    z_count = 32 if mesh.shape["fs"] == 128 else mesh.shape["fs"] // 4
    split = Mesh(
        mesh.devices.reshape(z_count, mesh.shape["fs"] // z_count, mesh.shape["tp"] // 2, 2),
        ("z", "y", "x", "c"),
    )
    fs, tp = ("z", "y"), ("x", "c")
    in_specs = (
        P(fs, None),
        P(),
        P(fs, tp),
        P(fs, tp),
        P(None, tp),
        P(tp, None, None),
        P(tp, None, None),
        P(tp),
        P(fs, tp),
        P(fs, tp),
        P(),
        P(fs, tp),
        P(fs, tp),
    )
    return jax.shard_map(
        layer, mesh=split, in_specs=in_specs, out_specs=P((*fs, *tp), None), check_vma=False
    )
```
